32 devices in a mesh: grp: 2 (over y), tp: 4 (over z), dp: 4 (over x, core).
Axes of the slice: x: 2, y: 2, z: 4, core: 2. Of those that a mesh axis runs over, the one named last changes fastest.
Arguments:
- stream: bfloat16 [256, 4096], P(('grp', 'tp'), 'dp'), parts along dimension 0, may hold values from -6 to 6
- lengths: int32 [16], P(('grp', 'dp')), parts along dimension 0, may hold values from 1 to 16, as said below
- input_norm_gain: float32 [2, 4096], P(None, 'dp'), may hold values from 0.1 to 1.9
- query_projection: bfloat16 [2, 4096, 2048], P(None, 'dp', 'tp'), may hold values from -0.09375 to 0.09375
- key_projection: bfloat16 [2, 4096, 2048], P(None, 'dp', 'tp'), may hold values from -0.09375 to 0.09375
- forget_gate_weight: bfloat16 [2, 4096, 2048], P(None, 'dp', 'tp'), may hold values from -0.09375 to 0.09375
- value_projection: bfloat16 [2, 4096, 4096], P(None, 'dp', 'tp'), may hold values from -0.09375 to 0.09375
- output_gate_weight: bfloat16 [2, 4096, 4096], P(None, 'dp', 'tp'), may hold values from -0.09375 to 0.09375
- forget_gate_bias: float32 [2, 2048], P(None, 'tp'), may hold values from -3 to 3
- extra_frame_decay: float32 [2, 256, 2048], P(None, ('grp', 'dp'), 'tp'), parts along dimension 1, may hold values from -0.7 to 0, as said below
- head_norm_gain: float32 [2, 512], replicated, may hold values from 0.1 to 1.9
- output_projection: bfloat16 [2, 4096, 4096], P(None, 'tp', 'dp'), may hold values from -0.09375 to 0.09375
- memory: float32 [2, 16, 2048, 512], P(None, ('grp', 'dp'), 'tp'), parts along dimension 1, may hold values from -6 to 6
Outputs:
- stream_out: bfloat16 [256, 4096], P(('grp', 'tp'), 'dp'), parts along dimension 0
- memory_out: float32 [2, 16, 2048, 512], P(None, ('grp', 'dp'), 'tp'), parts along dimension 1
The draws below stay inside these ranges and needn't reach their ends.
There are 2 independent parts, one for each index of `grp`. The reference program is written for one: setup_inputs(seed, part) draws one part's arguments, and reference() takes and returns one part's arrays. A program takes and returns all parts, laid end to end along the dimension named above; an argument that names none is the same for every part. Nothing has to cross between parts.
Inputs may be any that keep to these rules, and one draw needn't show every extreme that they name: `lengths`: live frames of each sequence; at least one sequence has all 16. `extra_frame_decay`: zero at most frames; at the others, for every key channel, a value from -0.7 to -0.22.
All inputs are finite; a program needn't handle non-finite values.
Results may differ from the reference program's by a relative error of at most 0.03.
Values may be sent and summed in bfloat16 or wider, within the bound.
A program may use at most 64 MiB of HBM per device.

```python
import jax
import jax.numpy as jnp
from jax import lax

D = 4096
HEADS = 8
KEY_DIM = 256
VALUE_DIM = 512
BLOCK_LEN = 16
BATCH = 8
TOKENS = 128
KEYS = 2048
VALUES = 4096
N_TP = 4
N_DP = 4


def draw_lengths(key, part):
    base_key, full_key, spot_key = jax.random.split(jax.random.fold_in(key, 23), 3)
    base = jax.random.randint(base_key, (BATCH,), 1, BLOCK_LEN // 2 + 4, dtype=jnp.int32)
    full_pick = jax.random.randint(full_key, (BATCH,), 0, 6, dtype=jnp.int32) == 0
    lengths = jnp.where(full_pick, BLOCK_LEN, base)
    spot = jax.random.randint(spot_key, (), 0, BATCH, dtype=jnp.int32)
    lengths = jnp.where(jnp.arange(BATCH, dtype=jnp.int32) == spot, BLOCK_LEN, lengths)
    return jnp.minimum(lengths, BLOCK_LEN).astype(jnp.int32)


def draw_extra_frame_decay(key, part):
    hit_key, amount_key = jax.random.split(jax.random.fold_in(key, 11))
    struck = jax.random.uniform(hit_key, (2, TOKENS, 1), jnp.float32) < 0.12
    amounts = jax.random.uniform(amount_key, (2, TOKENS, KEYS), jnp.float32, -0.7, -0.22)
    return jnp.where(struck, amounts, 0.0).astype(jnp.float32)


def block_levels(key, shape, cuts, low, high):
    def one(axis_at, parts):
        steps = jax.random.uniform(jax.random.fold_in(jax.random.fold_in(key, 6), axis_at), (parts,), jnp.float32, low / len(cuts), high / len(cuts))
        return jnp.repeat(jnp.exp(steps), shape[axis_at] // parts).reshape((-1,) + (1,) * (len(shape) - axis_at - 1))

    gain = one(*cuts[0])
    for cut in cuts[1:]:
        gain = gain * one(*cut)
    return gain


def bell_draw(rng, extent, scale, most, cuts=(), kind=jnp.bfloat16):
    level = block_levels(rng, extent, cuts, -0.22, 0.18) if cuts else 1.0
    values = jax.random.normal(rng, extent, jnp.float32) * scale * level
    return jnp.minimum(jnp.maximum(values, -most), most).astype(kind)


def setup_inputs(seed: int = 0, part: int = 0) -> dict:
    streams_of = jax.random.split(jax.random.key(seed), 14)
    part_splits = jax.random.split(jax.random.fold_in(streams_of[13], part), 14)
    return {
        "stream": bell_draw(part_splits[0], (TOKENS, D), 1.0, 6.0, ((0, 4), (1, 4))),
        "lengths": draw_lengths(jax.random.fold_in(jax.random.fold_in(streams_of[13], part), 71), part),
        "input_norm_gain": jnp.clip(1.0 + 0.18 * jax.random.normal(streams_of[2], (2, D), jnp.float32), 0.1, 1.9),
        "query_projection": bell_draw(streams_of[3], (2, D, KEYS), D ** -0.5, 0.09375, ((1, 4), (2, 4))),
        "key_projection": bell_draw(streams_of[4], (2, D, KEYS), D ** -0.5, 0.09375, ((1, 4), (2, 4))),
        "forget_gate_weight": bell_draw(streams_of[5], (2, D, KEYS), D ** -0.5, 0.09375, ((1, 4), (2, 4))),
        "value_projection": bell_draw(streams_of[6], (2, D, VALUES), D ** -0.5, 0.09375, ((1, 4), (2, 4))),
        "output_gate_weight": bell_draw(streams_of[7], (2, D, VALUES), D ** -0.5, 0.09375, ((1, 4), (2, 4))),
        "forget_gate_bias": jnp.clip(jax.random.uniform(streams_of[8], (2, KEYS), jnp.float32, -3.0, 3.0) * block_levels(streams_of[8], (2, KEYS), ((1, 4),), -0.4, 0.0), -3.0, 3.0),
        "extra_frame_decay": draw_extra_frame_decay(jax.random.fold_in(jax.random.fold_in(streams_of[13], part), 71), part),
        "head_norm_gain": jnp.clip(1.0 + 0.18 * jax.random.normal(streams_of[10], (2, VALUE_DIM), jnp.float32), 0.1, 1.9),
        "output_projection": bell_draw(streams_of[11], (2, VALUES, D), VALUES ** -0.5, 0.09375, ((1, 4), (2, 4))),
        "memory": bell_draw(part_splits[12], (2, BATCH, KEYS, VALUE_DIM), 1.0, 6.0, ((1, 4), (2, 4)), jnp.float32),
    }


EPS = 1e-06
TIME_CONSTANT = 16.0
HIGH = lax.Precision.HIGHEST

def recurrence(queries, keys_in, values_in, decay_logarithm, state_in):
    frames = queries.shape[1]
    totals = jnp.cumsum(decay_logarithm, axis=1)
    causal = (jnp.arange(frames)[:, None] >= jnp.arange(frames)[None, :])[None, :, :, None, None]
    spread = totals[:, :, None] - totals[:, None, :]
    decays = jnp.where(causal, jnp.exp(jnp.where(causal, spread, 0.0)), 0.0)
    scores = jnp.einsum('sihk,sijhk,sjhk->shij', queries, decays, keys_in, precision=HIGH)
    inner_part = jnp.einsum('shij,sjhv->sihv', scores, values_in, precision=HIGH)
    carried = jnp.einsum('sihk,shkv->sihv', queries * jnp.exp(totals), state_in, precision=HIGH)
    last_total = totals[:, -1]
    weighted = keys_in * jnp.exp(last_total[:, None] - totals)
    fresh_mem = jnp.exp(last_total)[..., None] * state_in + jnp.einsum('sjhk,sjhv->shkv', weighted, values_in, precision=HIGH)
    return (inner_part + carried, fresh_mem)

def split_sum(left_mat, right_mat, pieces):
    row_count = left_mat.shape[1] // pieces

    def add_piece(running, piece_idx):
        part = jnp.dot(lax.dynamic_slice_in_dim(left_mat, piece_idx * row_count, row_count, 1), lax.dynamic_slice_in_dim(right_mat, piece_idx * row_count, row_count, 0), preferred_element_type=jnp.float32)
        rounded = lax.optimization_barrier(part.astype(jnp.bfloat16))
        return (running + rounded.astype(jnp.float32), None)
    begin = jnp.zeros((left_mat.shape[0], right_mat.shape[1]), jnp.float32)
    running, _ = lax.scan(add_piece, begin, jnp.arange(pieces, dtype=jnp.int32))
    return running

def reference(stream, lengths, input_norm_gain, query_projection, key_projection, forget_gate_weight, value_projection, output_gate_weight, forget_gate_bias, extra_frame_decay, head_norm_gain, output_projection, memory):
    position = jnp.arange(BLOCK_LEN, dtype=jnp.int32)
    alive_mask = (position[None, :] < lengths[:, None]).astype(jnp.float32).reshape(TOKENS, 1)
    current = stream
    outputs = []
    for block_layer in range(2):
        residual = current.astype(jnp.float32)
        row_scale = lax.rsqrt(lax.optimization_barrier(jnp.mean(residual * residual, axis=1, keepdims=True)) + EPS)
        scaled = (residual * input_norm_gain[block_layer]).astype(jnp.bfloat16)
        queries = split_sum(scaled, query_projection[block_layer], N_DP) * row_scale * KEY_DIM ** (-0.5)
        keys_in = split_sum(scaled, key_projection[block_layer], N_DP) * row_scale * alive_mask
        forget_preactivation = split_sum(scaled, forget_gate_weight[block_layer], N_DP) * row_scale + forget_gate_bias[block_layer]
        values_in = split_sum(scaled, value_projection[block_layer], N_DP) * row_scale
        gate_pre = split_sum(scaled, output_gate_weight[block_layer], N_DP) * row_scale
        decay_logarithm = (jax.nn.log_sigmoid(forget_preactivation) / TIME_CONSTANT + extra_frame_decay[block_layer]) * alive_mask
        read_out, fresh_mem = recurrence(queries.reshape(BATCH, BLOCK_LEN, HEADS, KEY_DIM), keys_in.reshape(BATCH, BLOCK_LEN, HEADS, KEY_DIM), values_in.reshape(BATCH, BLOCK_LEN, HEADS, VALUE_DIM), decay_logarithm.reshape(BATCH, BLOCK_LEN, HEADS, KEY_DIM), memory[block_layer].reshape(BATCH, HEADS, KEY_DIM, VALUE_DIM))
        normed = read_out * lax.rsqrt(lax.optimization_barrier(jnp.mean(read_out * read_out, axis=3, keepdims=True)) + EPS) * head_norm_gain[block_layer]
        gated = (normed.reshape(TOKENS, VALUES) * jax.nn.silu(gate_pre) * alive_mask).astype(jnp.bfloat16)
        mixer_out = split_sum(gated, output_projection[block_layer], N_TP).astype(jnp.bfloat16)
        current = (residual + mixer_out.astype(jnp.float32)).astype(jnp.bfloat16)
        outputs.append(fresh_mem.reshape(BATCH, KEYS, VALUE_DIM))
    return (current, jnp.stack(outputs))
```

```python
import functools

import jax
import jax.numpy as jnp
from jax import lax
from jax.experimental import pallas as pl
from jax.experimental.pallas import tpu as pltpu
from jax.sharding import PartitionSpec as P

D = 4096
KEY_DIM = 256
VALUE_DIM = 512
BLOCK_LEN = 16


EPS = 1e-06
TIME_CONSTANT = 16.0
HIGH = lax.Precision.HIGHEST


def for_sending(array):
    return jax.tree.map(lambda a: a.astype(jnp.bfloat16) if a.dtype == jnp.float32 else a, array)


def swapped(value, axis, distance):
    mask = 2**distance
    pairs = [(source, source ^ mask) for source in range(lax.axis_size(axis))]
    return lax.ppermute(value, axis, pairs)


def recurrence(queries, keys_in, values_in, decay_logarithm, state_in):
    frames = queries.shape[1]
    totals = jnp.cumsum(decay_logarithm, axis=1)
    causal = (jnp.arange(frames)[:, None] >= jnp.arange(frames)[None, :])[None, :, :, None, None]
    spread = totals[:, :, None] - totals[:, None, :]
    decays = jnp.where(causal, jnp.exp(jnp.where(causal, spread, 0.0)), 0.0)
    scores = jnp.einsum("sihk,sijhk,sjhk->shij", queries, decays, keys_in, precision=HIGH)
    inner_part = jnp.einsum("shij,sjhv->sihv", scores, values_in, precision=HIGH)
    carried = jnp.einsum("sihk,shkv->sihv", queries * jnp.exp(totals), state_in, precision=HIGH)
    last_total = totals[:, -1]
    weighted = keys_in * jnp.exp(last_total[:, None] - totals)
    fresh_mem = jnp.exp(last_total)[..., None] * state_in + jnp.einsum(
        "sjhk,sjhv->shkv", weighted, values_in, precision=HIGH
    )
    return (inner_part + carried, fresh_mem)


def local(
    stream,
    lengths,
    input_norm_gain,
    query_projection,
    key_projection,
    forget_gate_weight,
    value_projection,
    output_gate_weight,
    forget_gate_bias,
    extra_frame_decay,
    head_norm_gain,
    output_projection,
    memory,
):
    key_local = query_projection.shape[2]
    value_local = value_projection.shape[2]
    local_heads = max(1, key_local // KEY_DIM)
    key_width = key_local // local_heads
    paired = key_local < KEY_DIM
    seq_local = lengths.shape[0]
    own_tokens = seq_local * BLOCK_LEN
    tp_spot = lax.axis_index("tp")
    position = jnp.arange(BLOCK_LEN, dtype=jnp.int32)
    alive_mask = (position[None, :] < lengths[:, None]).astype(jnp.float32).reshape(own_tokens, 1)
    current = stream
    outputs = []
    for block_layer in range(2):
        residual = current.astype(jnp.float32)
        gathered = lax.all_gather(current, "tp", axis=0, tiled=True)
        wide_res = gathered.astype(jnp.float32)
        scaled = (wide_res * input_norm_gain[block_layer]).astype(jnp.bfloat16)
        own_power = lax.psum_scatter(
            jnp.sum(wide_res * wide_res, axis=1), "dp", scatter_dimension=0, tiled=True
        )
        row_scale = lax.rsqrt(own_power / D + EPS)[:, None]
        joined = jnp.concatenate(
            [
                query_projection[block_layer],
                key_projection[block_layer],
                forget_gate_weight[block_layer],
                value_projection[block_layer],
                output_gate_weight[block_layer],
            ],
            axis=1,
        )
        summed = (
            lax.psum_scatter(
                jnp.dot(scaled, joined, preferred_element_type=jnp.float32).astype(jnp.bfloat16),
                "dp",
                scatter_dimension=0,
                tiled=True,
            ).astype(jnp.float32)
            * row_scale
        )
        second_cut = 2 * key_local
        third_cut = 3 * key_local
        fourth_cut = 3 * key_local + value_local
        queries = summed[:, :key_local] * KEY_DIM ** (-0.5)
        keys_in = summed[:, key_local:second_cut] * alive_mask
        forget_preactivation = summed[:, second_cut:third_cut] + forget_gate_bias[block_layer]
        values_in = summed[:, third_cut:fourth_cut]
        gate_pre = summed[:, fourth_cut:]
        decay_logarithm = (
            jax.nn.log_sigmoid(forget_preactivation) / TIME_CONSTANT
            + extra_frame_decay[block_layer]
        ) * alive_mask
        is_upper = tp_spot % 2 == 1
        if paired:
            partner = swapped(for_sending(values_in), "tp", 0).astype(values_in.dtype)
            values_full = jnp.where(
                is_upper,
                jnp.concatenate([partner, values_in], 1),
                jnp.concatenate([values_in, partner], 1),
            )
        else:
            values_full = values_in
        read_out, fresh_mem = recurrence(
            queries.reshape(seq_local, BLOCK_LEN, local_heads, key_width),
            keys_in.reshape(seq_local, BLOCK_LEN, local_heads, key_width),
            values_full.reshape(seq_local, BLOCK_LEN, local_heads, VALUE_DIM),
            decay_logarithm.reshape(seq_local, BLOCK_LEN, local_heads, key_width),
            memory[block_layer].reshape(seq_local, local_heads, key_width, VALUE_DIM),
        )
        if paired:
            read_out = read_out + swapped(for_sending(read_out), "tp", 0).astype(read_out.dtype)
        normed = (
            read_out
            * lax.rsqrt(jnp.mean(read_out * read_out, axis=3, keepdims=True) + EPS)
            * head_norm_gain[block_layer]
        )
        flat = normed.reshape(own_tokens, local_heads * VALUE_DIM)
        if paired:
            flat = lax.dynamic_slice_in_dim(flat, tp_spot % 2 * value_local, value_local, 1)
        gated = (flat * jax.nn.silu(gate_pre) * alive_mask).astype(jnp.bfloat16)
        partials = jnp.dot(
            lax.all_gather(gated, "dp", axis=0, tiled=True),
            output_projection[block_layer],
            preferred_element_type=jnp.float32,
        )
        mixer_out = lax.psum_scatter(
            partials.astype(jnp.bfloat16), "tp", scatter_dimension=0, tiled=True
        )
        current = (residual + mixer_out.astype(jnp.float32)).astype(jnp.bfloat16)
        outputs.append(fresh_mem.reshape(seq_local, key_local, VALUE_DIM))
    return (current, jnp.stack(outputs))


MESH = pl.DeviceIdType.MESH
LAYERS = 2
SEQS = 2
HIDDEN = -1e30


def fused_kernel(
    n_tp,
    stream,
    lengths,
    gain_in,
    wq_in,
    wk_in,
    wf_in,
    wv_in,
    wg_in,
    bias_in,
    extra_in,
    hgain_in,
    wo_in,
    memory_in,
    stream_out,
    memory_out,
    w,
    wo,
    mem,
    fresh,
    gain,
    bias,
    extra,
    hgain,
    ag,
    xs,
    pb,
    r1,
    s2,
    r2,
    sq_s,
    sq_r,
    gbuf,
    rs_s,
    rs_r,
    w_sem,
    wo_sem,
    mem_sem,
    out_sem,
    small_sem,
    ag_ss,
    ag_rs,
    p1_ss,
    p1_rs,
    p2_ss,
    p2_rs,
    sq_ss,
    sq_rs,
    g_ss,
    g_rs,
    o_ss,
    o_rs,
):
    tp = lax.axis_index("tp")
    dp = lax.axis_index("dp")
    chip = dp // 2
    core = dp % 2
    rows = stream.shape[0]
    chunk = w.shape[3]
    chunks = w.shape[1]
    key_local = wq_in.shape[2]
    value_local = wv_in.shape[2]
    heads = key_local // KEY_DIM
    own = rows

    dp_peers = [chip * 2 + 1 - core, (1 - chip) * 2 + core, (1 - chip) * 2 + 1 - core]
    tp_offsets = list(range(1, n_tp))

    def tp_to(offset):
        return lax.rem(tp + offset, n_tp)

    def tp_from(offset):
        return lax.rem(tp + n_tp - offset, n_tp)

    first = pltpu.make_async_copy(stream, ag.at[0, tp], small_sem.at[0])
    first.start()
    gain_copy = pltpu.make_async_copy(gain_in, gain, small_sem.at[1])
    gain_copy.start()

    def weight_copies(l):
        pieces = []
        for source in (wq_in, wk_in, wf_in, wv_in, wg_in):
            for at in range(0, source.shape[2], chunk):
                pieces.append(source.at[l, :, pl.ds(at, chunk)])
        return [
            pltpu.make_async_copy(piece, w.at[l, c], w_sem.at[l, c])
            for c, piece in enumerate(pieces)
        ]

    for copy in weight_copies(0):
        copy.start()

    barrier = pltpu.get_barrier_semaphore()
    for offset in tp_offsets:
        pl.semaphore_signal(barrier, inc=1, device_id={"tp": tp_to(offset)}, device_id_type=MESH)
    for peer in dp_peers:
        pl.semaphore_signal(barrier, inc=1, device_id={"dp": peer}, device_id_type=MESH)
    others = [
        pltpu.make_async_copy(bias_in, bias, small_sem.at[2]),
        pltpu.make_async_copy(extra_in, extra, small_sem.at[3]),
        pltpu.make_async_copy(hgain_in, hgain, small_sem.at[4]),
    ]
    for copy in others:
        copy.start()
    pl.semaphore_wait(barrier, len(tp_offsets) + len(dp_peers))
    first.wait()
    gain_copy.wait()
    for copy in others:
        copy.wait()

    row_of = lax.broadcasted_iota(jnp.int32, (own, 1), 0)
    seq_of = row_of // BLOCK_LEN
    place = row_of - seq_of * BLOCK_LEN
    live_count = jnp.where(seq_of == 0, lengths[0], lengths[1])
    alive = jnp.where(place < live_count, 1.0, 0.0).astype(jnp.float32)
    lane = lax.broadcasted_iota(jnp.int32, (own, 128), 1)

    def mem_copy(l):
        return pltpu.make_async_copy(memory_in.at[l], mem.at[l], mem_sem.at[l])

    def wo_copy(l):
        return pltpu.make_async_copy(wo_in.at[l], wo.at[l], wo_sem.at[l])

    def fresh_copy(l):
        return pltpu.make_async_copy(fresh.at[l], memory_out.at[l], out_sem.at[l])

    def layer(l, carry):
        gather = []
        for offset in tp_offsets:
            copy = pltpu.make_async_remote_copy(
                src_ref=ag.at[l, tp],
                dst_ref=ag.at[l, tp],
                send_sem=ag_ss.at[l, offset],
                recv_sem=ag_rs.at[l, offset],
                device_id={"tp": tp_to(offset)},
                device_id_type=MESH,
            )
            copy.start()
            gather.append(copy)
        gain_row = gain[pl.ds(l, 1), :]
        diag = lax.broadcasted_iota(jnp.int32, (own, 128), 0)

        def prepare(source):
            wide = ag[l, source].astype(jnp.float32)
            xs[pl.ds(source * rows, rows), :] = (wide * gain_row).astype(jnp.bfloat16)
            power = jnp.sum(wide * wide, axis=1, keepdims=True)
            return jnp.sum(jnp.where(lane == diag + source * rows, power, 0.0), axis=0, keepdims=True)

        powers = prepare(tp)
        for offset in tp_offsets:
            pltpu.make_async_remote_copy(
                src_ref=ag.at[l, tp],
                dst_ref=ag.at[l, tp_from(offset)],
                send_sem=ag_ss.at[l, offset],
                recv_sem=ag_rs.at[l, offset],
                device_id={"tp": tp_to(offset)},
                device_id_type=MESH,
            ).wait_recv()
            powers = powers + prepare(tp_from(offset))
        sq_s[l] = jnp.broadcast_to(powers, (8, 128))

        @pl.when(l == 0)
        def _():
            mem_copy(0).start()
            wo_copy(0).start()

        def stage_one(c):
            return pltpu.make_async_remote_copy(
                src_ref=pb.at[l, c, :, 1 - core],
                dst_ref=r1.at[l, c],
                send_sem=p1_ss.at[l, c],
                recv_sem=p1_rs.at[l, c],
                device_id={"dp": dp_peers[0]},
                device_id_type=MESH,
            )

        def stage_two(c):
            return pltpu.make_async_remote_copy(
                src_ref=s2.at[l, c],
                dst_ref=r2.at[l, c],
                send_sem=p2_ss.at[l, c],
                recv_sem=p2_rs.at[l, c],
                device_id={"dp": dp_peers[1]},
                device_id_type=MESH,
            )

        def pass_on(c):
            stage_one(c).wait_recv()
            s2[l, c] = (
                pb[l, c, 1 - chip, core].astype(jnp.float32)
                + r1[l, c, 1 - chip].astype(jnp.float32)
            ).astype(jnp.bfloat16)
            stage_two(c).start()

        squares = []
        weights = weight_copies(l)
        for c in range(chunks):
            weights[c].wait()
            part = jnp.dot(xs[...], w[l, c], preferred_element_type=jnp.float32)
            pb[l, c] = part.astype(jnp.bfloat16).reshape(2, 2, rows, chunk)
            stage_one(c).start()
            if c == 0:
                for k, peer in enumerate(dp_peers):
                    copy = pltpu.make_async_remote_copy(
                        src_ref=sq_s.at[l],
                        dst_ref=sq_r.at[l, k],
                        send_sem=sq_ss.at[l, k],
                        recv_sem=sq_rs.at[l, k],
                        device_id={"dp": peer},
                        device_id_type=MESH,
                    )
                    copy.start()
                    squares.append(copy)
            else:
                pass_on(c - 1)
        pass_on(chunks - 1)

        @pl.when(l == 0)
        def _():
            for copy in weight_copies(1):
                copy.start()
            mem_copy(1).start()
            wo_copy(1).start()

        total = sq_s[l]
        for k in range(len(dp_peers)):
            squares[k].wait_recv()
            total = total + sq_r[l, k]
        own_power = jnp.sum(
            jnp.where(lane == diag + dp * own, total[0:1, :], 0.0), axis=1, keepdims=True
        )
        row_scale = lax.rsqrt(own_power / D + EPS)

        def summed(c):
            stage_two(c).wait_recv()
            both = pb[l, c, chip, core].astype(jnp.float32) + r1[l, c, chip].astype(jnp.float32)
            return (both + r2[l, c].astype(jnp.float32)) * row_scale

        key_chunks = key_local // chunk
        value_chunks = value_local // chunk

        def taken(start, count):
            parts = [summed(c) for c in range(start, start + count)]
            return parts[0] if count == 1 else jnp.concatenate(parts, axis=1)

        queries = taken(0, key_chunks) * KEY_DIM ** (-0.5)
        keys_in = taken(key_chunks, key_chunks) * alive
        forget = taken(2 * key_chunks, key_chunks) + bias[pl.ds(l, 1), :]
        log_sig = jnp.minimum(forget, 0.0) - jnp.log(1.0 + jnp.exp(-jnp.abs(forget)))
        totals = (log_sig / TIME_CONSTANT + extra[l]) * alive
        step = 1
        while step < BLOCK_LEN:
            totals = totals + jnp.where(place >= step, pltpu.roll(totals, step, 0), 0.0)
            step *= 2

        def each_seq(array, j):
            return jnp.concatenate(
                [
                    jnp.broadcast_to(
                        array[s * BLOCK_LEN + j : s * BLOCK_LEN + j + 1, :],
                        (BLOCK_LEN, array.shape[1]),
                    )
                    for s in range(SEQS)
                ],
                axis=0,
            )

        scores = [jnp.zeros((own, 128), jnp.float32) for _ in range(heads)]
        for j in range(BLOCK_LEN):
            decay = jnp.exp(jnp.where(place >= j, totals - each_seq(totals, j), HIDDEN))
            product = queries * decay * each_seq(keys_in, j)
            for h in range(heads):
                column = jnp.sum(
                    product[:, h * KEY_DIM : (h + 1) * KEY_DIM], axis=1, keepdims=True
                )
                scores[h] = jnp.where(lane == seq_of * BLOCK_LEN + j, column, scores[h])
        carried_q = (queries * jnp.exp(totals)).astype(jnp.bfloat16)
        last = each_seq(totals, BLOCK_LEN - 1)
        weighted = (keys_in * jnp.exp(last - totals)).astype(jnp.bfloat16)
        last_decay = jnp.exp(last)

        mem_copy(l).wait()
        carried = []
        for h in range(heads):
            span = slice(h * KEY_DIM, (h + 1) * KEY_DIM)
            carried.append(
                jnp.concatenate(
                    [
                        jnp.dot(
                            carried_q[s * BLOCK_LEN : (s + 1) * BLOCK_LEN, span],
                            mem[l, s, span, :].astype(jnp.bfloat16),
                            preferred_element_type=jnp.float32,
                        )
                        for s in range(SEQS)
                    ],
                    axis=0,
                )
            )
        values_in = taken(3 * key_chunks, value_chunks).astype(jnp.bfloat16)
        normed = []
        for h in range(heads):
            read = carried[h] + jnp.dot(
                scores[h][:, :own].astype(jnp.bfloat16),
                values_in[:, h * VALUE_DIM : (h + 1) * VALUE_DIM],
                preferred_element_type=jnp.float32,
            )
            normed.append(
                read
                * lax.rsqrt(jnp.mean(read * read, axis=1, keepdims=True) + EPS)
                * hgain[pl.ds(l, 1), :]
            )
        gate_pre = taken(3 * key_chunks + value_chunks, value_chunks)
        flat = jnp.concatenate(normed, axis=1)
        gbuf[l, dp] = (flat * (gate_pre * jax.nn.sigmoid(gate_pre)) * alive).astype(jnp.bfloat16)

        def gated_copy(k, source):
            return pltpu.make_async_remote_copy(
                src_ref=gbuf.at[l, dp],
                dst_ref=gbuf.at[l, source],
                send_sem=g_ss.at[l, k],
                recv_sem=g_rs.at[l, k],
                device_id={"dp": dp_peers[k]},
                device_id_type=MESH,
            )

        for k in (1, 2, 0):
            gated_copy(k, dp).start()

        def partial_copy(dest):
            return pltpu.make_async_remote_copy(
                src_ref=rs_s.at[l, dest],
                dst_ref=rs_r.at[l, tp],
                send_sem=o_ss.at[l, dest],
                recv_sem=o_rs.at[l, tp],
                device_id={"tp": dest},
                device_id_type=MESH,
            )

        def project(side):
            left = gbuf[l, pl.ds(2 * side, 2)].reshape(2 * rows, value_local)
            out = jnp.dot(left, wo[l], preferred_element_type=jnp.float32)
            rs_s[l, pl.ds(2 * side, 2)] = out.astype(jnp.bfloat16).reshape(2, rows, out.shape[1])
            for i in range(2):
                dest = 2 * side + i

                @pl.when(dest != tp)
                def _():
                    partial_copy(dest).start()

        def update(s, h):
            span = slice(h * KEY_DIM, (h + 1) * KEY_DIM)
            ahead = slice(s * BLOCK_LEN, (s + 1) * BLOCK_LEN)
            grown = lax.dot_general(
                weighted[ahead, span],
                values_in[ahead, h * VALUE_DIM : (h + 1) * VALUE_DIM],
                (((0,), (0,)), ((), ())),
                preferred_element_type=jnp.float32,
            )
            kept = jnp.transpose(
                jnp.broadcast_to(last_decay[s * BLOCK_LEN : s * BLOCK_LEN + 1, span], (128, KEY_DIM))
            )
            kept = jnp.concatenate([kept] * (VALUE_DIM // 128), axis=1)
            fresh[l, s, span, :] = kept * mem[l, s, span, :] + grown

        wo_copy(l).wait()
        gated_copy(0, dp_peers[0]).wait_recv()
        project(chip)
        for s in range(SEQS):
            for h in range(heads):
                update(s, h)
        fresh_copy(l).start()
        gated_copy(1, dp_peers[1]).wait_recv()
        gated_copy(2, dp_peers[2]).wait_recv()
        project(1 - chip)

        mixed = rs_s[l, tp].astype(jnp.float32)
        for offset in tp_offsets:
            source = tp_from(offset)
            pltpu.make_async_remote_copy(
                src_ref=rs_s.at[l, source],
                dst_ref=rs_r.at[l, source],
                send_sem=o_ss.at[l, source],
                recv_sem=o_rs.at[l, source],
                device_id={"tp": source},
                device_id_type=MESH,
            ).wait_recv()
            mixed = mixed + rs_r[l, source].astype(jnp.float32)
        mixed = mixed.astype(jnp.bfloat16).astype(jnp.float32)
        ag[l + 1, tp] = (ag[l, tp].astype(jnp.float32) + mixed).astype(jnp.bfloat16)

        for copy in gather + squares:
            copy.wait_send()
        for c in range(chunks):
            stage_one(c).wait_send()
            stage_two(c).wait_send()
        for k in range(len(dp_peers)):
            gated_copy(k, dp).wait_send()
        for offset in tp_offsets:
            partial_copy(tp_to(offset)).wait_send()
        return carry

    lax.fori_loop(0, LAYERS, layer, 0)
    done = pltpu.make_async_copy(ag.at[LAYERS, tp], stream_out, small_sem.at[0])
    done.start()
    for l in range(LAYERS):
        fresh_copy(l).wait()
    done.wait()


def fused(n_tp, *args):
    stream, wq, wv, wo_all, memory = args[0], args[3], args[6], args[11], args[12]
    rows, features = stream.shape
    key_local, value_local = wq.shape[2], wv.shape[2]
    chunk = KEY_DIM * 2
    chunks = (3 * key_local + 2 * value_local) // chunk
    n_dp = 4
    bf, f32 = jnp.bfloat16, jnp.float32
    dma = pltpu.SemaphoreType.DMA
    anywhere = pl.BlockSpec(memory_space=pl.ANY)
    in_specs = [anywhere] * len(args)
    in_specs[1] = pl.BlockSpec(memory_space=pltpu.SMEM)
    return pl.pallas_call(
        functools.partial(fused_kernel, n_tp),
        out_shape=(
            jax.ShapeDtypeStruct(stream.shape, bf),
            jax.ShapeDtypeStruct(memory.shape, f32),
        ),
        in_specs=in_specs,
        out_specs=(anywhere, anywhere),
        scratch_shapes=[
            pltpu.VMEM((LAYERS, chunks, features, chunk), bf),
            pltpu.VMEM(wo_all.shape, bf),
            pltpu.VMEM(memory.shape, f32),
            pltpu.VMEM(memory.shape, f32),
            pltpu.VMEM(args[2].shape, f32),
            pltpu.VMEM(args[8].shape, f32),
            pltpu.VMEM(args[9].shape, f32),
            pltpu.VMEM(args[10].shape, f32),
            pltpu.VMEM((LAYERS + 1, n_tp, rows, features), bf),
            pltpu.VMEM((n_tp * rows, features), bf),
            pltpu.VMEM((LAYERS, chunks, 2, 2, rows, chunk), bf),
            pltpu.VMEM((LAYERS, chunks, 2, rows, chunk), bf),
            pltpu.VMEM((LAYERS, chunks, rows, chunk), bf),
            pltpu.VMEM((LAYERS, chunks, rows, chunk), bf),
            pltpu.VMEM((LAYERS, 8, 128), f32),
            pltpu.VMEM((LAYERS, n_dp - 1, 8, 128), f32),
            pltpu.VMEM((LAYERS, n_dp, rows, value_local), bf),
            pltpu.VMEM((LAYERS, n_tp, rows, features), bf),
            pltpu.VMEM((LAYERS, n_tp, rows, features), bf),
            dma((LAYERS, chunks)),
            dma((LAYERS,)),
            dma((LAYERS,)),
            dma((LAYERS,)),
            dma((5,)),
            dma((LAYERS, n_tp)),
            dma((LAYERS, n_tp)),
            dma((LAYERS, chunks)),
            dma((LAYERS, chunks)),
            dma((LAYERS, chunks)),
            dma((LAYERS, chunks)),
            dma((LAYERS, n_dp - 1)),
            dma((LAYERS, n_dp - 1)),
            dma((LAYERS, n_dp - 1)),
            dma((LAYERS, n_dp - 1)),
            dma((LAYERS, n_tp)),
            dma((LAYERS, n_tp)),
        ],
        compiler_params=pltpu.CompilerParams(
            collective_id=0, has_side_effects=True, vmem_limit_bytes=60 * 1024 * 1024
        ),
    )(*args)


def body(*args):
    stream, wq = args[0], args[3]
    n_tp, n_dp = lax.axis_size("tp"), lax.axis_size("dp")
    fits = (
        n_dp == 4
        and n_tp == 4
        and args[1].shape[0] == SEQS
        and stream.shape[0] == SEQS * BLOCK_LEN
        and wq.shape[2] % (2 * KEY_DIM) == 0
    )
    return fused(n_tp, *args) if fits else local(*args)


def solution(mesh):
    placed = (
        P(("grp", "tp"), "dp"),
        P(("grp", "dp")),
        P(None, "dp"),
        P(None, "dp", "tp"),
        P(None, "dp", "tp"),
        P(None, "dp", "tp"),
        P(None, "dp", "tp"),
        P(None, "dp", "tp"),
        P(None, "tp"),
        P(None, ("grp", "dp"), "tp"),
        P(),
        P(None, "tp", "dp"),
        P(None, ("grp", "dp"), "tp", None),
    )
    return jax.shard_map(
        body,
        mesh=mesh,
        in_specs=placed,
        out_specs=(P(("grp", "tp"), "dp"), P(None, ("grp", "dp"), "tp", None)),
        check_vma=False,
    )
```

```python
import functools

import jax
import jax.numpy as jnp
from jax import lax
from jax.experimental import pallas as pl
from jax.experimental.pallas import tpu as pltpu
from jax.sharding import PartitionSpec as P

D = 4096
KEY_DIM = 256
VALUE_DIM = 512
BLOCK_LEN = 16


EPS = 1e-06
TIME_CONSTANT = 16.0
HIGH = lax.Precision.HIGHEST


def for_sending(array):
    return jax.tree.map(lambda a: a.astype(jnp.bfloat16) if a.dtype == jnp.float32 else a, array)


def swapped(value, axis, distance):
    mask = 2**distance
    pairs = [(source, source ^ mask) for source in range(lax.axis_size(axis))]
    return lax.ppermute(value, axis, pairs)


def recurrence(queries, keys_in, values_in, decay_logarithm, state_in):
    frames = queries.shape[1]
    totals = jnp.cumsum(decay_logarithm, axis=1)
    causal = (jnp.arange(frames)[:, None] >= jnp.arange(frames)[None, :])[None, :, :, None, None]
    spread = totals[:, :, None] - totals[:, None, :]
    decays = jnp.where(causal, jnp.exp(jnp.where(causal, spread, 0.0)), 0.0)
    scores = jnp.einsum("sihk,sijhk,sjhk->shij", queries, decays, keys_in, precision=HIGH)
    inner_part = jnp.einsum("shij,sjhv->sihv", scores, values_in, precision=HIGH)
    carried = jnp.einsum("sihk,shkv->sihv", queries * jnp.exp(totals), state_in, precision=HIGH)
    last_total = totals[:, -1]
    weighted = keys_in * jnp.exp(last_total[:, None] - totals)
    fresh_mem = jnp.exp(last_total)[..., None] * state_in + jnp.einsum(
        "sjhk,sjhv->shkv", weighted, values_in, precision=HIGH
    )
    return (inner_part + carried, fresh_mem)


def local(
    stream,
    lengths,
    input_norm_gain,
    query_projection,
    key_projection,
    forget_gate_weight,
    value_projection,
    output_gate_weight,
    forget_gate_bias,
    extra_frame_decay,
    head_norm_gain,
    output_projection,
    memory,
):
    key_local = query_projection.shape[2]
    value_local = value_projection.shape[2]
    local_heads = max(1, key_local // KEY_DIM)
    key_width = key_local // local_heads
    paired = key_local < KEY_DIM
    seq_local = lengths.shape[0]
    own_tokens = seq_local * BLOCK_LEN
    tp_spot = lax.axis_index("tp")
    position = jnp.arange(BLOCK_LEN, dtype=jnp.int32)
    alive_mask = (position[None, :] < lengths[:, None]).astype(jnp.float32).reshape(own_tokens, 1)
    current = stream
    outputs = []
    for block_layer in range(2):
        residual = current.astype(jnp.float32)
        gathered = lax.all_gather(current, "tp", axis=0, tiled=True)
        wide_res = gathered.astype(jnp.float32)
        scaled = (wide_res * input_norm_gain[block_layer]).astype(jnp.bfloat16)
        own_power = lax.psum_scatter(
            jnp.sum(wide_res * wide_res, axis=1), "dp", scatter_dimension=0, tiled=True
        )
        row_scale = lax.rsqrt(own_power / D + EPS)[:, None]
        joined = jnp.concatenate(
            [
                query_projection[block_layer],
                key_projection[block_layer],
                forget_gate_weight[block_layer],
                value_projection[block_layer],
                output_gate_weight[block_layer],
            ],
            axis=1,
        )
        summed = (
            lax.psum_scatter(
                jnp.dot(scaled, joined, preferred_element_type=jnp.float32).astype(jnp.bfloat16),
                "dp",
                scatter_dimension=0,
                tiled=True,
            ).astype(jnp.float32)
            * row_scale
        )
        second_cut = 2 * key_local
        third_cut = 3 * key_local
        fourth_cut = 3 * key_local + value_local
        queries = summed[:, :key_local] * KEY_DIM ** (-0.5)
        keys_in = summed[:, key_local:second_cut] * alive_mask
        forget_preactivation = summed[:, second_cut:third_cut] + forget_gate_bias[block_layer]
        values_in = summed[:, third_cut:fourth_cut]
        gate_pre = summed[:, fourth_cut:]
        decay_logarithm = (
            jax.nn.log_sigmoid(forget_preactivation) / TIME_CONSTANT
            + extra_frame_decay[block_layer]
        ) * alive_mask
        is_upper = tp_spot % 2 == 1
        if paired:
            partner = swapped(for_sending(values_in), "tp", 0).astype(values_in.dtype)
            values_full = jnp.where(
                is_upper,
                jnp.concatenate([partner, values_in], 1),
                jnp.concatenate([values_in, partner], 1),
            )
        else:
            values_full = values_in
        read_out, fresh_mem = recurrence(
            queries.reshape(seq_local, BLOCK_LEN, local_heads, key_width),
            keys_in.reshape(seq_local, BLOCK_LEN, local_heads, key_width),
            values_full.reshape(seq_local, BLOCK_LEN, local_heads, VALUE_DIM),
            decay_logarithm.reshape(seq_local, BLOCK_LEN, local_heads, key_width),
            memory[block_layer].reshape(seq_local, local_heads, key_width, VALUE_DIM),
        )
        if paired:
            read_out = read_out + swapped(for_sending(read_out), "tp", 0).astype(read_out.dtype)
        normed = (
            read_out
            * lax.rsqrt(jnp.mean(read_out * read_out, axis=3, keepdims=True) + EPS)
            * head_norm_gain[block_layer]
        )
        flat = normed.reshape(own_tokens, local_heads * VALUE_DIM)
        if paired:
            flat = lax.dynamic_slice_in_dim(flat, tp_spot % 2 * value_local, value_local, 1)
        gated = (flat * jax.nn.silu(gate_pre) * alive_mask).astype(jnp.bfloat16)
        partials = jnp.dot(
            lax.all_gather(gated, "dp", axis=0, tiled=True),
            output_projection[block_layer],
            preferred_element_type=jnp.float32,
        )
        mixer_out = lax.psum_scatter(
            partials.astype(jnp.bfloat16), "tp", scatter_dimension=0, tiled=True
        )
        current = (residual + mixer_out.astype(jnp.float32)).astype(jnp.bfloat16)
        outputs.append(fresh_mem.reshape(seq_local, key_local, VALUE_DIM))
    return (current, jnp.stack(outputs))


MESH = pl.DeviceIdType.MESH
LAYERS = 2
SEQS = 2
PARTS = 2
LAG = 4
HIDDEN = -1e30


def fused_kernel(
    n_tp,
    stream,
    lengths,
    gain_in,
    wq_in,
    wk_in,
    wf_in,
    wv_in,
    wg_in,
    bias_in,
    extra_in,
    hgain_in,
    wo_in,
    memory_in,
    stream_out,
    memory_out,
    w,
    wo,
    mem,
    fresh,
    gain,
    bias,
    extra,
    hgain,
    ag,
    xs,
    pb,
    r1,
    s2,
    r2,
    sq_s,
    sq_r,
    gbuf,
    rs_s,
    rs_r,
    w_sem,
    wo_sem,
    mem_sem,
    out_sem,
    small_sem,
    stream_sem,
    ag_ss,
    ag_rs,
    p1_ss,
    p1_rs,
    p2_ss,
    p2_rs,
    sq_ss,
    sq_rs,
    g_ss,
    g_rs,
    o_ss,
    o_rs,
):
    tp = lax.axis_index("tp")
    dp = lax.axis_index("dp")
    chip = dp // 2
    core = dp % 2
    rows = stream.shape[0]
    chunk = w.shape[3]
    chunks = w.shape[1]
    key_local = wq_in.shape[2]
    value_local = wv_in.shape[2]
    heads = key_local // KEY_DIM
    own = rows
    parts = ag.shape[1]
    width = ag.shape[4]

    dp_peers = [chip * 2 + 1 - core, (1 - chip) * 2 + core, (1 - chip) * 2 + 1 - core]
    tp_offsets = list(range(1, n_tp))

    def tp_to(offset):
        return lax.rem(tp + offset, n_tp)

    def tp_from(offset):
        return lax.rem(tp + n_tp - offset, n_tp)

    def stream_copy(b):
        return pltpu.make_async_copy(
            stream.at[:, pl.ds(b * width, width)], ag.at[0, b, tp], stream_sem.at[b]
        )

    for b in range(parts):
        stream_copy(b).start()
    gain_copy = pltpu.make_async_copy(gain_in, gain, small_sem.at[1])
    gain_copy.start()

    def weight_copies(l):
        pieces = []
        for source in (wq_in, wk_in, wf_in, wv_in, wg_in):
            for at in range(0, source.shape[2], chunk):
                pieces.append(source.at[l, :, pl.ds(at, chunk)])
        return [
            pltpu.make_async_copy(piece, w.at[l, c], w_sem.at[l, c])
            for c, piece in enumerate(pieces)
        ]

    others = [
        pltpu.make_async_copy(bias_in, bias, small_sem.at[2]),
        pltpu.make_async_copy(extra_in, extra, small_sem.at[3]),
        pltpu.make_async_copy(hgain_in, hgain, small_sem.at[4]),
    ]

    barrier = pltpu.get_barrier_semaphore()
    for offset in tp_offsets:
        pl.semaphore_signal(barrier, inc=1, device_id={"tp": tp_to(offset)}, device_id_type=MESH)
    for peer in dp_peers:
        pl.semaphore_signal(barrier, inc=1, device_id={"dp": peer}, device_id_type=MESH)
    for copy in weight_copies(0) + others:
        copy.start()
    pl.semaphore_wait(barrier, len(tp_offsets) + len(dp_peers))

    def gather_copy(l, b, offset, source):
        return pltpu.make_async_remote_copy(
            src_ref=ag.at[l, b, tp],
            dst_ref=ag.at[l, b, source],
            send_sem=ag_ss.at[l, b, offset],
            recv_sem=ag_rs.at[l, b, offset],
            device_id={"tp": tp_to(offset)},
            device_id_type=MESH,
        )

    def gather_start(l, b):
        for offset in tp_offsets:
            gather_copy(l, b, offset, tp).start()

    for b in range(parts):
        stream_copy(b).wait()
        gather_start(0, b)
    gain_copy.wait()

    row_of = lax.broadcasted_iota(jnp.int32, (own, 1), 0)
    seq_of = row_of // BLOCK_LEN
    place = row_of - seq_of * BLOCK_LEN
    live_count = jnp.where(seq_of == 0, lengths[0], lengths[1])
    alive = jnp.where(place < live_count, 1.0, 0.0).astype(jnp.float32)
    lane = lax.broadcasted_iota(jnp.int32, (own, 128), 1)

    def mem_copy(l):
        return pltpu.make_async_copy(memory_in.at[l], mem.at[l], mem_sem.at[l])

    def wo_copy(l):
        return pltpu.make_async_copy(wo_in.at[l], wo.at[l], wo_sem.at[l])

    def fresh_copy(l):
        return pltpu.make_async_copy(fresh.at[l], memory_out.at[l], out_sem.at[l])

    def layer(l, carry):
        gain_row = gain[pl.ds(l, 1), :]
        diag = lax.broadcasted_iota(jnp.int32, (own, 128), 0)

        def prepare(b, source):
            columns = slice(b * width, (b + 1) * width)
            wide = ag[l, b, source].astype(jnp.float32)
            xs[pl.ds(source * rows, rows), columns] = (wide * gain_row[:, columns]).astype(
                jnp.bfloat16
            )
            power = jnp.sum(wide * wide, axis=1, keepdims=True)
            return jnp.sum(jnp.where(lane == diag + source * rows, power, 0.0), axis=0, keepdims=True)

        powers = jnp.zeros((1, 128), jnp.float32)
        for b in range(parts):
            powers = powers + prepare(b, tp)
        for b in range(parts):
            for offset in tp_offsets:
                gather_copy(l, b, offset, tp_from(offset)).wait_recv()
                powers = powers + prepare(b, tp_from(offset))
        sq_s[l] = jnp.broadcast_to(powers, (8, 128))

        @pl.when(l == 0)
        def _():
            mem_copy(0).start()
            wo_copy(0).start()

        def stage_one(c):
            return pltpu.make_async_remote_copy(
                src_ref=pb.at[l, c, :, 1 - core],
                dst_ref=r1.at[l, c],
                send_sem=p1_ss.at[l, c],
                recv_sem=p1_rs.at[l, c],
                device_id={"dp": dp_peers[0]},
                device_id_type=MESH,
            )

        def stage_two(c):
            return pltpu.make_async_remote_copy(
                src_ref=s2.at[l, c],
                dst_ref=r2.at[l, c],
                send_sem=p2_ss.at[l, c],
                recv_sem=p2_rs.at[l, c],
                device_id={"dp": dp_peers[1]},
                device_id_type=MESH,
            )

        def pass_on(c):
            stage_one(c).wait_recv()
            s2[l, c] = (
                pb[l, c, 1 - chip, core].astype(jnp.float32)
                + r1[l, c, 1 - chip].astype(jnp.float32)
            ).astype(jnp.bfloat16)
            stage_two(c).start()

        squares = []
        weights = weight_copies(l)
        for c in range(chunks):
            weights[c].wait()
            part = jnp.dot(xs[...], w[l, c], preferred_element_type=jnp.float32)
            pb[l, c] = part.astype(jnp.bfloat16).reshape(2, 2, rows, chunk)
            stage_one(c).start()
            if c == 0:
                for k, peer in enumerate(dp_peers):
                    copy = pltpu.make_async_remote_copy(
                        src_ref=sq_s.at[l],
                        dst_ref=sq_r.at[l, k],
                        send_sem=sq_ss.at[l, k],
                        recv_sem=sq_rs.at[l, k],
                        device_id={"dp": peer},
                        device_id_type=MESH,
                    )
                    copy.start()
                    squares.append(copy)
            if c >= LAG:
                pass_on(c - LAG)
        for c in range(max(0, chunks - LAG), chunks):
            pass_on(c)

        @pl.when(l == 0)
        def _():
            for copy in weight_copies(1):
                copy.start()
            mem_copy(1).start()
            wo_copy(1).start()

        @pl.when(l == 0)
        def _():
            for copy in others:
                copy.wait()

        total = sq_s[l]
        for k in range(len(dp_peers)):
            squares[k].wait_recv()
            total = total + sq_r[l, k]
        own_power = jnp.sum(
            jnp.where(lane == diag + dp * own, total[0:1, :], 0.0), axis=1, keepdims=True
        )
        row_scale = lax.rsqrt(own_power / D + EPS)

        def summed(c):
            stage_two(c).wait_recv()
            both = pb[l, c, chip, core].astype(jnp.float32) + r1[l, c, chip].astype(jnp.float32)
            return (both + r2[l, c].astype(jnp.float32)) * row_scale

        key_chunks = key_local // chunk
        value_chunks = value_local // chunk

        def taken(start, count):
            parts = [summed(c) for c in range(start, start + count)]
            return parts[0] if count == 1 else jnp.concatenate(parts, axis=1)

        queries = taken(0, key_chunks) * KEY_DIM ** (-0.5)
        keys_in = taken(key_chunks, key_chunks) * alive
        forget = taken(2 * key_chunks, key_chunks) + bias[pl.ds(l, 1), :]
        log_sig = jnp.minimum(forget, 0.0) - jnp.log(1.0 + jnp.exp(-jnp.abs(forget)))
        totals = (log_sig / TIME_CONSTANT + extra[l]) * alive
        step = 1
        while step < BLOCK_LEN:
            totals = totals + jnp.where(place >= step, pltpu.roll(totals, step, 0), 0.0)
            step *= 2

        def each_seq(array, j):
            return jnp.concatenate(
                [
                    jnp.broadcast_to(
                        array[s * BLOCK_LEN + j : s * BLOCK_LEN + j + 1, :],
                        (BLOCK_LEN, array.shape[1]),
                    )
                    for s in range(SEQS)
                ],
                axis=0,
            )

        scores = [jnp.zeros((own, 128), jnp.float32) for _ in range(heads)]
        for j in range(BLOCK_LEN):
            decay = jnp.exp(jnp.where(place >= j, totals - each_seq(totals, j), HIDDEN))
            product = queries * decay * each_seq(keys_in, j)
            for h in range(heads):
                column = jnp.sum(
                    product[:, h * KEY_DIM : (h + 1) * KEY_DIM], axis=1, keepdims=True
                )
                scores[h] = jnp.where(lane == seq_of * BLOCK_LEN + j, column, scores[h])
        carried_q = (queries * jnp.exp(totals)).astype(jnp.bfloat16)
        last = each_seq(totals, BLOCK_LEN - 1)
        weighted = (keys_in * jnp.exp(last - totals)).astype(jnp.bfloat16)
        last_decay = jnp.exp(last)

        mem_copy(l).wait()
        carried = []
        for h in range(heads):
            span = slice(h * KEY_DIM, (h + 1) * KEY_DIM)
            carried.append(
                jnp.concatenate(
                    [
                        jnp.dot(
                            carried_q[s * BLOCK_LEN : (s + 1) * BLOCK_LEN, span],
                            mem[l, s, span, :].astype(jnp.bfloat16),
                            preferred_element_type=jnp.float32,
                        )
                        for s in range(SEQS)
                    ],
                    axis=0,
                )
            )
        values_in = taken(3 * key_chunks, value_chunks).astype(jnp.bfloat16)
        normed = []
        for h in range(heads):
            read = carried[h] + jnp.dot(
                scores[h][:, :own].astype(jnp.bfloat16),
                values_in[:, h * VALUE_DIM : (h + 1) * VALUE_DIM],
                preferred_element_type=jnp.float32,
            )
            normed.append(
                read
                * lax.rsqrt(jnp.mean(read * read, axis=1, keepdims=True) + EPS)
                * hgain[pl.ds(l, 1), :]
            )
        gate_pre = taken(3 * key_chunks + value_chunks, value_chunks)
        flat = jnp.concatenate(normed, axis=1)
        gbuf[l, dp] = (flat * (gate_pre * jax.nn.sigmoid(gate_pre)) * alive).astype(jnp.bfloat16)

        def gated_copy(k, source):
            return pltpu.make_async_remote_copy(
                src_ref=gbuf.at[l, dp],
                dst_ref=gbuf.at[l, source],
                send_sem=g_ss.at[l, k],
                recv_sem=g_rs.at[l, k],
                device_id={"dp": dp_peers[k]},
                device_id_type=MESH,
            )

        for k in (1, 2, 0):
            gated_copy(k, dp).start()

        def partial_copy(b, dest, source):
            return pltpu.make_async_remote_copy(
                src_ref=rs_s.at[l, b, dest],
                dst_ref=rs_r.at[l, b, source],
                send_sem=o_ss.at[l, b, dest],
                recv_sem=o_rs.at[l, b, source],
                device_id={"tp": dest},
                device_id_type=MESH,
            )

        def project(side, b):
            left = gbuf[l, pl.ds(2 * side, 2)].reshape(2 * rows, value_local)
            out = jnp.dot(
                left, wo[l, :, b * width : (b + 1) * width], preferred_element_type=jnp.float32
            )
            rs_s[l, b, pl.ds(2 * side, 2)] = out.astype(jnp.bfloat16).reshape(2, rows, width)
            for i in range(2):
                dest = 2 * side + i

                @pl.when(dest != tp)
                def _():
                    partial_copy(b, dest, tp).start()

        def update(s, h):
            span = slice(h * KEY_DIM, (h + 1) * KEY_DIM)
            ahead = slice(s * BLOCK_LEN, (s + 1) * BLOCK_LEN)
            grown = lax.dot_general(
                weighted[ahead, span],
                values_in[ahead, h * VALUE_DIM : (h + 1) * VALUE_DIM],
                (((0,), (0,)), ((), ())),
                preferred_element_type=jnp.float32,
            )
            kept = jnp.transpose(
                jnp.broadcast_to(last_decay[s * BLOCK_LEN : s * BLOCK_LEN + 1, span], (128, KEY_DIM))
            )
            kept = jnp.concatenate([kept] * (VALUE_DIM // 128), axis=1)
            fresh[l, s, span, :] = (kept * mem[l, s, span, :] + grown).astype(jnp.bfloat16)

        wo_copy(l).wait()
        gated_copy(0, dp_peers[0]).wait_recv()
        for b in range(parts):
            project(chip, b)
        for s in range(SEQS):
            for h in range(heads):
                update(s, h)
        fresh_copy(l).start()
        gated_copy(1, dp_peers[1]).wait_recv()
        gated_copy(2, dp_peers[2]).wait_recv()
        for b in range(parts):
            project(1 - chip, b)

        for b in range(parts):
            mixed = rs_s[l, b, tp].astype(jnp.float32)
            for offset in tp_offsets:
                source = tp_from(offset)
                partial_copy(b, source, source).wait_recv()
                mixed = mixed + rs_r[l, b, source].astype(jnp.float32)
            mixed = mixed.astype(jnp.bfloat16).astype(jnp.float32)
            ag[l + 1, b, tp] = (ag[l, b, tp].astype(jnp.float32) + mixed).astype(jnp.bfloat16)

            @pl.when(l + 1 < LAYERS)
            def _():
                gather_start(l + 1, b)

        for copy in squares:
            copy.wait_send()
        for c in range(chunks):
            stage_one(c).wait_send()
            stage_two(c).wait_send()
        for k in range(len(dp_peers)):
            gated_copy(k, dp).wait_send()
        for b in range(parts):
            for offset in tp_offsets:
                gather_copy(l, b, offset, tp).wait_send()
                partial_copy(b, tp_to(offset), tp).wait_send()
        return carry

    lax.fori_loop(0, LAYERS, layer, 0)
    done = [
        pltpu.make_async_copy(
            ag.at[LAYERS, b, tp], stream_out.at[:, pl.ds(b * width, width)], stream_sem.at[b]
        )
        for b in range(parts)
    ]
    for copy in done:
        copy.start()
    for l in range(LAYERS):
        fresh_copy(l).wait()
    for copy in done:
        copy.wait()


def fused(n_tp, *args):
    stream, wq, wv, wo_all, memory = args[0], args[3], args[6], args[11], args[12]
    rows, features = stream.shape
    key_local, value_local = wq.shape[2], wv.shape[2]
    chunk = KEY_DIM * 2
    chunks = (3 * key_local + 2 * value_local) // chunk
    n_dp = 4
    bf, f32 = jnp.bfloat16, jnp.float32
    dma = pltpu.SemaphoreType.DMA
    anywhere = pl.BlockSpec(memory_space=pl.ANY)
    in_specs = [anywhere] * len(args)
    in_specs[1] = pl.BlockSpec(memory_space=pltpu.SMEM)
    return pl.pallas_call(
        functools.partial(fused_kernel, n_tp),
        out_shape=(
            jax.ShapeDtypeStruct(stream.shape, bf),
            jax.ShapeDtypeStruct(memory.shape, bf),
        ),
        in_specs=in_specs,
        out_specs=(anywhere, anywhere),
        scratch_shapes=[
            pltpu.VMEM((LAYERS, chunks, features, chunk), bf),
            pltpu.VMEM(wo_all.shape, bf),
            pltpu.VMEM(memory.shape, f32),
            pltpu.VMEM(memory.shape, bf),
            pltpu.VMEM(args[2].shape, f32),
            pltpu.VMEM(args[8].shape, f32),
            pltpu.VMEM(args[9].shape, f32),
            pltpu.VMEM(args[10].shape, f32),
            pltpu.VMEM((LAYERS + 1, PARTS, n_tp, rows, features // PARTS), bf),
            pltpu.VMEM((n_tp * rows, features), bf),
            pltpu.VMEM((LAYERS, chunks, 2, 2, rows, chunk), bf),
            pltpu.VMEM((LAYERS, chunks, 2, rows, chunk), bf),
            pltpu.VMEM((LAYERS, chunks, rows, chunk), bf),
            pltpu.VMEM((LAYERS, chunks, rows, chunk), bf),
            pltpu.VMEM((LAYERS, 8, 128), f32),
            pltpu.VMEM((LAYERS, n_dp - 1, 8, 128), f32),
            pltpu.VMEM((LAYERS, n_dp, rows, value_local), bf),
            pltpu.VMEM((LAYERS, PARTS, n_tp, rows, features // PARTS), bf),
            pltpu.VMEM((LAYERS, PARTS, n_tp, rows, features // PARTS), bf),
            dma((LAYERS, chunks)),
            dma((LAYERS,)),
            dma((LAYERS,)),
            dma((LAYERS,)),
            dma((5,)),
            dma((PARTS,)),
            dma((LAYERS, PARTS, n_tp)),
            dma((LAYERS, PARTS, n_tp)),
            dma((LAYERS, chunks)),
            dma((LAYERS, chunks)),
            dma((LAYERS, chunks)),
            dma((LAYERS, chunks)),
            dma((LAYERS, n_dp - 1)),
            dma((LAYERS, n_dp - 1)),
            dma((LAYERS, n_dp - 1)),
            dma((LAYERS, n_dp - 1)),
            dma((LAYERS, PARTS, n_tp)),
            dma((LAYERS, PARTS, n_tp)),
        ],
        compiler_params=pltpu.CompilerParams(
            collective_id=0, has_side_effects=True, vmem_limit_bytes=60 * 1024 * 1024
        ),
    )(*args)


def body(*args):
    stream, wq = args[0], args[3]
    n_tp, n_dp = lax.axis_size("tp"), lax.axis_size("dp")
    fits = (
        n_dp == 4
        and n_tp == 4
        and args[1].shape[0] == SEQS
        and stream.shape[0] == SEQS * BLOCK_LEN
        and wq.shape[2] % (2 * KEY_DIM) == 0
    )
    if not fits:
        return local(*args)
    current, memories = fused(n_tp, *args)
    return current, memories.astype(jnp.float32)


def solution(mesh):
    placed = (
        P(("grp", "tp"), "dp"),
        P(("grp", "dp")),
        P(None, "dp"),
        P(None, "dp", "tp"),
        P(None, "dp", "tp"),
        P(None, "dp", "tp"),
        P(None, "dp", "tp"),
        P(None, "dp", "tp"),
        P(None, "tp"),
        P(None, ("grp", "dp"), "tp"),
        P(),
        P(None, "tp", "dp"),
        P(None, ("grp", "dp"), "tp", None),
    )
    return jax.shard_map(
        body,
        mesh=mesh,
        in_specs=placed,
        out_specs=(P(("grp", "tp"), "dp"), P(None, ("grp", "dp"), "tp", None)),
        check_vma=False,
    )
```
